128 devices in a mesh: sp: 16 (over z, y), dp: 8 (over x, core).
Axes of the slice: x: 4, y: 4, z: 4, core: 2. Of those that a mesh axis runs over, the one named last changes fastest.
Arguments:
- query_first: bfloat16 [8, 2048, 1024], P('dp', 'sp'), may hold values from -200 to 200
- key_first: bfloat16 [8, 2048, 1024], P('dp', 'sp'), may hold values from -8 to 8
- query_second: bfloat16 [8, 2048, 1024], P('dp', 'sp'), may hold values from -200 to 200
- key_second: bfloat16 [8, 2048, 1024], P('dp', 'sp'), may hold values from -8 to 8
- value_rows: bfloat16 [8, 2048, 2048], P('dp', 'sp'), may hold values from -6 to 6
- mix_lambda: float32 [16], replicated, may hold values from 0.3 to 0.8
- head_gain: float32 [128], replicated, may hold values from 0.1 to 1.9
- residual: bfloat16 [8, 2048, 2048], P('dp', 'sp'), may hold values from -6 to 6
- out_weight: bfloat16 [2048, 2048], replicated, may hold values from -0.125 to 0.125
- norm_gain: float32 [2048], replicated, may hold values from 0.1 to 1.9
- routes: int32 [8, 2048, 4], P('dp', 'sp'), may hold values from 0 to 127, all different within a row; in each aligned block of 128 rows (0 to 127, 128 to 255, ..., all dimensions but the last counted through in order) at most 6 rows name the same one
- route_weights: float32 [8, 2048, 4], P('dp', 'sp'), may hold values from 0.1 to 1
- gate_weight: bfloat16 [128, 2048, 1024], P(('sp', 'dp')), may hold values from -0.375 to 0.375
- up_weight: bfloat16 [128, 2048, 1024], P(('sp', 'dp')), may hold values from -0.375 to 0.375
- down_weight: bfloat16 [128, 1024, 2048], P(('sp', 'dp')), may hold values from -0.046875 to 0.046875
Outputs:
- layer_out: bfloat16 [8, 2048, 2048], P('dp', 'sp')
The draws below stay inside these ranges and needn't reach their ends.
Inputs may be any that keep to these rules, and one draw needn't show every extreme that they name: `routes`: within the rows of one device (aligned blocks of 128 positions of a sequence) no expert is named more than 6 times, a bound that some block reaches.
All inputs are finite; a program needn't handle non-finite values.
Results may differ from the reference program's by a relative error of at most 0.0075.
Values may be sent and summed in bfloat16 or wider, within the bound.
No kernel may reach another device: no remote copies, remote signals or barrier semaphores. Data moves between devices by JAX's collectives and lax.ppermute only.
A program may use at most 128 MiB of HBM per device.

```python
import math
import jax
import jax.numpy as jnp
import numpy as np
from jax import lax

D = 2048
H = 16
HD = 64
HV = 128
FF = 1024
TOPK = 4
TOK_DEV = 128
LENGTH = 2048
SEQS = 8
EXPERTS = 128
CAP = 6
N_SP = 16
N_DP = 8


def drawn(key, which):
    shape = (SEQS, LENGTH, H * HD)
    keys = jnp.clip(jax.random.normal(jax.random.fold_in(key, 10 + which), shape, jnp.float32) * 1.3, -8.0, 8.0)
    queries = jnp.clip(jax.random.normal(jax.random.fold_in(key, 20 + which), shape, jnp.float32) * 1.3, -8.0, 8.0)
    return (queries, keys)


def draw_query_first(key, part):
    return drawn(key, 0)[0].astype(jnp.bfloat16)


def draw_key_first(key, part):
    return drawn(key, 0)[1].astype(jnp.bfloat16)


def draw_query_second(key, part):
    return drawn(key, 1)[0].astype(jnp.bfloat16)


def draw_key_second(key, part):
    return drawn(key, 1)[1].astype(jnp.bfloat16)


def block_scale(key, dims, cuts, least, top_value):
    factor_of = 1.0
    for dim, blocks in cuts:
        draws = jax.random.uniform(jax.random.fold_in(jax.random.fold_in(key, 6), dim), (blocks,), jnp.float32, least / len(cuts), top_value / len(cuts))
        factor_of = factor_of * jnp.repeat(jnp.exp(draws), dims[dim] // blocks).reshape((-1,) + (1,) * (len(dims) - 1 - dim))
    return factor_of


def shared_out(own_key, own, number, rows, amount, top, bound, slope):
    ranking = jax.random.permutation(own_key, amount)
    heavy_load, ordinary = load_shares(amount, rows * top, bound, slope, True), load_shares(amount, rows * top, bound, slope, False)
    places = jnp.arange(amount)

    def named(lengths, offset_by):
        used = int((lengths > 0).sum())
        fixed = max(1, used // 4)
        passed = fixed + (places - fixed + offset_by * (used - fixed)) % max(1, amount - fixed)
        return jnp.zeros((amount,), jnp.int32).at[ranking[jnp.where(places < fixed, places, passed)]].set(jnp.asarray(lengths, jnp.int32))

    lengths = jnp.where(number % 4 == 0, named(heavy_load, number // 4), named(ordinary, number - number // 4 - 1))
    mixed = jax.random.permutation(jax.random.fold_in(own, 3), amount)
    giver, sink = mixed[0:amount // 2 * 2:2], mixed[1:amount // 2 * 2:2]
    slack = jnp.minimum(lengths[giver] - 1, bound - lengths[sink]) // 2
    slack = jnp.where((giver == ranking[0]) | (sink == ranking[0]) | (lengths[sink] == 0), 0, jnp.maximum(slack, 0))
    passed = jax.random.randint(jax.random.fold_in(own, 4), (amount // 2,), 0, 1 << 20) % (slack + 1)
    lengths = lengths.at[giver].add(-passed).at[sink].add(passed)
    labels = jnp.searchsorted(jnp.cumsum(lengths), jnp.arange(rows * top), side="right").astype(jnp.int32)
    listing = labels.reshape(top, rows).T
    listing = listing[jax.random.permutation(jax.random.fold_in(own, 1), rows)]
    offset_by = jax.random.randint(jax.random.fold_in(own, 2), (rows, 1), 0, top)
    return jnp.take_along_axis(listing, (jnp.arange(top)[None, :] + offset_by) % top, axis=1)


def load_shares(amount, total, most, skew, full):
    weights = [(1 << 20) // math.isqrt(grade ** skew) + 1 for grade in range(1, amount + 1)]
    largest = most if full else min(most, max(-(-total // amount), total * weights[0] // sum(weights)))
    least = 1 if total - largest >= amount - 1 else 0
    holding, surplus = [largest] + [least] * (amount - 1), total - largest - least * (amount - 1)
    while surplus > 0:
        candidates = [i for i in range(1, amount) if holding[i] < largest] or [i for i in range(1, amount) if holding[i] < most]
        pool, remaining = sum([weights[i] for i in candidates]), surplus
        for i in candidates:
            addition = min(most - holding[i], max(1, remaining * weights[i] // pool), surplus)
            holding[i] = holding[i] + addition
            surplus = surplus - addition
    return np.array(holding)


def bell_draw(rng, extent, deviation, bound, split=(), kind=jnp.bfloat16):
    values = jax.random.normal(rng, extent, jnp.float32) * deviation
    if len(split) > 0:
        values = block_scale(rng, extent, split, -0.22, 0.18) * values
    return jnp.clip(values, min=-bound, max=bound).astype(kind)


def setup_inputs(seed: int = 0) -> dict:
    key_list = jax.random.split(jax.random.key(seed), 16)
    query_first = draw_query_first(jax.random.fold_in(key_list[15], 71), 0)
    key_first = draw_key_first(jax.random.fold_in(key_list[15], 71), 0)
    query_second = draw_query_second(jax.random.fold_in(key_list[15], 71), 0)
    key_second = draw_key_second(jax.random.fold_in(key_list[15], 71), 0)
    value_rows = bell_draw(key_list[4], (SEQS, LENGTH, H * HV), 1.0, 6.0, ((0, 8), (1, 16)))
    mix_lambda = jnp.clip(jax.random.uniform(key_list[5], (H,), jnp.float32, 0.3, 0.8), 0.3, 0.8)
    head_gain = jnp.clip(1.0 + 0.18 * jax.random.normal(key_list[6], (HV,), jnp.float32), 0.1, 1.9)
    residual = bell_draw(key_list[7], (SEQS, LENGTH, D), 1.0, 6.0, ((0, 8), (1, 16)))
    out_weight = bell_draw(key_list[8], (H * HV, D), (H * HV) ** -0.5, 0.125)
    norm_gain = jnp.clip(1.0 + 0.18 * jax.random.normal(key_list[9], (D,), jnp.float32), 0.1, 1.9)
    routes_keys = jax.random.split(jax.random.fold_in(key_list[10], 1), SEQS * LENGTH // TOK_DEV)
    routes_turns = jax.random.permutation(jax.random.fold_in(key_list[10], 3), SEQS * LENGTH // TOK_DEV)
    routes = jax.vmap(lambda own, number: shared_out(jax.random.fold_in(key_list[10], 2), own, number, TOK_DEV, EXPERTS, TOPK, CAP, 2))(routes_keys, routes_turns).reshape((SEQS, LENGTH, TOPK))
    route_weights = jnp.clip(0.1 + 0.9 * jax.random.uniform(key_list[11], (SEQS, LENGTH, TOPK), jnp.float32) ** block_scale(key_list[11], (SEQS, LENGTH, TOPK), ((0, 8), (1, 16)), -0.2, 0.2), 0.1, 1.0)
    gate_weight = bell_draw(key_list[12], (EXPERTS, D, FF), (D // 9) ** -0.5, 0.375, ((0, 128),))
    up_weight = bell_draw(key_list[13], (EXPERTS, D, FF), (D // 9) ** -0.5, 0.375, ((0, 128),))
    down_weight = bell_draw(key_list[14], (EXPERTS, FF, D), (16 * FF) ** -0.5, 0.046875, ((0, 128),))
    return dict(query_first=query_first, key_first=key_first, query_second=query_second, key_second=key_second, value_rows=value_rows, mix_lambda=mix_lambda, head_gain=head_gain, residual=residual, out_weight=out_weight, norm_gain=norm_gain, routes=routes, route_weights=route_weights, gate_weight=gate_weight, up_weight=up_weight, down_weight=down_weight)


def head_attention(operands):
    query_one, key_one, query_two, key_two, value_head, weight_two, head_gain = operands
    length = query_one.shape[0]
    qblock = min(length, max(512, length // 16))
    scale = HD ** (-0.5)
    keypos = jnp.arange(length, dtype=jnp.int32)

    def block(start):
        rows = start * qblock + jnp.arange(qblock, dtype=jnp.int32)
        q_one = lax.dynamic_slice_in_dim(query_one, (start * qblock).astype(jnp.int32), qblock, 0)
        q_two = lax.dynamic_slice_in_dim(query_two, (start * qblock).astype(jnp.int32), qblock, 0)
        score_one = jnp.dot(q_one, key_one.T, preferred_element_type=jnp.float32) * scale
        score_two = jnp.dot(q_two, key_two.T, preferred_element_type=jnp.float32) * scale
        visible = keypos[None, :] <= rows[:, None]
        prob_one = jax.nn.softmax(jnp.where(visible, score_one, -1e+30), axis=-1)
        prob_two = jax.nn.softmax(jnp.where(visible, score_two, -1e+30), axis=-1)
        mixture = (prob_one - weight_two * prob_two).astype(jnp.bfloat16)
        head_raw = jnp.dot(mixture, value_head, preferred_element_type=jnp.float32)
        factor = lax.rsqrt(lax.optimization_barrier(jnp.mean(head_raw * head_raw, axis=-1, keepdims=True)) + 1e-06)
        return (head_raw * factor * head_gain).astype(jnp.bfloat16)
    return lax.map(block, jnp.arange(length // qblock, dtype=jnp.int32)).reshape(length, HV)

def reference(query_first, key_first, query_second, key_second, value_rows, mix_lambda, head_gain, residual, out_weight, norm_gain, routes, route_weights, gate_weight, up_weight, down_weight):

    def by_head(array, width):
        return array.reshape(SEQS, LENGTH, H, width).transpose(0, 2, 1, 3).reshape(SEQS * H, LENGTH, width)
    gains = jnp.broadcast_to(head_gain, (SEQS * H, HV))
    heads = lax.map(head_attention, (by_head(query_first, HD), by_head(key_first, HD), by_head(query_second, HD), by_head(key_second, HD), by_head(value_rows, HV), jnp.tile(mix_lambda, SEQS), gains))
    head_out = heads.reshape(SEQS, H, LENGTH, HV).transpose(0, 2, 1, 3).reshape(SEQS * LENGTH, H * HV)
    attn = jnp.dot(head_out, out_weight, preferred_element_type=jnp.float32)
    mixed = residual.reshape(SEQS * LENGTH, D).astype(jnp.float32) + attn
    normed = (mixed * lax.rsqrt(lax.optimization_barrier(jnp.mean(mixed * mixed, axis=-1, keepdims=True)) + 1e-06) * norm_gain).astype(jnp.bfloat16)
    expert_ids = routes.reshape(-1)
    weights = route_weights.reshape(-1)
    total = expert_ids.shape[0]
    order = jnp.argsort(expert_ids, stable=True).astype(jnp.int32)
    counts = jnp.bincount(expert_ids, length=EXPERTS).astype(jnp.int32)
    starts = (jnp.cumsum(counts) - counts).astype(jnp.int32)
    room = CAP * N_SP * N_DP
    offsets = jnp.arange(room, dtype=jnp.int32)

    def expert_step(acc, operands):
        expert, w_gate, w_up, w_down = operands
        slots = jnp.minimum(starts[expert] + offsets, total - 1)
        valid = offsets < counts[expert]
        picks = order[slots]
        tokens = picks // TOPK
        rows = normed[tokens]
        gate = jnp.dot(rows, w_gate, preferred_element_type=jnp.float32)
        upper = jnp.dot(rows, w_up, preferred_element_type=jnp.float32)
        clamped = jnp.minimum(gate, 7.0)
        hidden = ((jnp.clip(upper, -7.0, 7.0) + 1.0) * clamped * jax.nn.sigmoid(1.702 * clamped)).astype(jnp.bfloat16)
        expert_out = jnp.dot(hidden, w_down, preferred_element_type=jnp.float32).astype(jnp.bfloat16)
        scaled = jnp.where(valid, weights[picks], 0.0)[:, None] * expert_out.astype(jnp.float32)
        return (acc.at[tokens].add(scaled), None)
    routed, _ = lax.scan(expert_step, jnp.zeros((SEQS * LENGTH, D), jnp.float32), (jnp.arange(EXPERTS, dtype=jnp.int32), gate_weight, up_weight, down_weight))
    return (mixed + routed).astype(jnp.bfloat16).reshape(SEQS, LENGTH, D)
```

```python
import functools

import jax
import jax.numpy as jnp
from jax import lax
from jax.experimental import pallas as pl
from jax.experimental.pallas import tpu as pltpu
from jax.sharding import PartitionSpec as P

BF = jnp.bfloat16
F32 = jnp.float32
LANES = 128
SLOTS = 6
ROWS = 8
MIB = 1024 * 1024


def dot(a, b, dims=((1,), (0,))):
    return lax.dot_general(a, b, (dims, ((), ())), preferred_element_type=F32)


def vmem_specs(count):
    return [pl.BlockSpec(memory_space=pltpu.VMEM)] * count


def pack_kernel(q1_ref, k1_ref, q2_ref, k2_ref, v_ref, out_ref):
    tok = q1_ref.shape[0]
    heads = v_ref.shape[1] // LANES
    half = LANES // 2
    for h in range(heads):
        rows = slice(h * tok, (h + 1) * tok)
        cols = slice(h * half, (h + 1) * half)
        out_ref[rows, 0:LANES] = jnp.concatenate([q1_ref[:, cols], q2_ref[:, cols]], axis=1)
        out_ref[rows, LANES : 2 * LANES] = jnp.concatenate(
            [k1_ref[:, cols], k2_ref[:, cols]], axis=1
        )
        out_ref[rows, 2 * LANES : 3 * LANES] = v_ref[:, h * LANES : (h + 1) * LANES]


def pack_heads(q1, k1, q2, k2, v):
    tok = q1.shape[0]
    heads = v.shape[1] // LANES
    return pl.pallas_call(
        pack_kernel,
        out_shape=jax.ShapeDtypeStruct((heads * tok, 3 * LANES), BF),
        in_specs=vmem_specs(5),
        out_specs=pl.BlockSpec(memory_space=pltpu.VMEM),
        compiler_params=pltpu.CompilerParams(vmem_limit_bytes=8 * MIB),
        name="pack_heads",
    )(q1, k1, q2, k2, v)


def attention_kernel(lam_ref, gain_ref, qkv_ref, out_ref, *, block):
    length = qkv_ref.shape[0]
    half = LANES // 2
    scale = (half**-0.5) * 1.4426950408889634
    lane = lax.broadcasted_iota(jnp.int32, (block, LANES), 1)
    causal = lax.broadcasted_iota(jnp.int32, (2 * block, block), 1) <= (
        lax.broadcasted_iota(jnp.int32, (2 * block, block), 0) & (block - 1)
    )
    lam = lam_ref[0, 0]
    gain = gain_ref[...]
    for step in range(length // block):
        rows = slice(step * block, (step + 1) * block)
        queries = qkv_ref[rows, 0:LANES]
        zero = jnp.zeros_like(queries)
        both = jnp.concatenate(
            [jnp.where(lane < half, queries, zero), jnp.where(lane < half, zero, queries)], axis=0
        )
        scores = []
        for c in range(step + 1):
            keys = qkv_ref[c * block : (c + 1) * block, LANES : 2 * LANES]
            s = dot(both, keys, ((1,), (1,)))
            if c == step:
                s = jnp.where(causal, s, -1e30)
            scores.append(s)
        top = functools.reduce(jnp.maximum, scores)
        top = jnp.max(top, axis=1, keepdims=True)
        total = None
        raw = None
        for c in range(step + 1):
            p = jnp.exp2((scores[c] - top) * scale)
            total = p if total is None else total + p
            values = qkv_ref[c * block : (c + 1) * block, 2 * LANES : 3 * LANES]
            part = dot(p.astype(BF), values)
            raw = part if raw is None else raw + part
        total = jnp.sum(total, axis=1, keepdims=True)
        normal = raw / total
        head = normal[:block] - lam * normal[block:]
        factor = lax.rsqrt(jnp.mean(head * head, axis=1, keepdims=True) + 1e-06)
        out_ref[rows, :] = (head * factor * gain).astype(BF)


def attention(lam, gain, qkv):
    length = qkv.shape[0]
    return pl.pallas_call(
        functools.partial(attention_kernel, block=256),
        out_shape=jax.ShapeDtypeStruct((length, LANES), BF),
        in_specs=[pl.BlockSpec(memory_space=pltpu.SMEM)] + vmem_specs(2),
        out_specs=pl.BlockSpec(memory_space=pltpu.VMEM),
        compiler_params=pltpu.CompilerParams(vmem_limit_bytes=24 * MIB),
        name="attention",
    )(lam, gain, qkv)


def route_kernel(routes_ref, weights_ref, send_ref, mix_ref):
    topk, tok = routes_ref.shape
    experts = send_ref.shape[0] // ROWS
    expert = lax.broadcasted_iota(jnp.int32, (experts, tok), 0)
    named = jnp.zeros((experts, tok), F32)
    weight = jnp.zeros((experts, tok), F32)
    for k in range(topk):
        hit = expert == routes_ref[k : k + 1, :]
        named = jnp.where(hit, 1.0, named)
        weight = jnp.where(hit, weights_ref[k : k + 1, :], weight)
    before = lax.broadcasted_iota(jnp.int32, (tok, tok), 0) < lax.broadcasted_iota(
        jnp.int32, (tok, tok), 1
    )
    rank = dot(named.astype(BF), jnp.where(before, 1.0, 0.0).astype(BF))
    slot = jnp.where(named > 0.0, rank, -9.0)
    high = weight.astype(BF)
    low = (weight - high.astype(F32)).astype(BF)

    def spread(x):
        x = jnp.broadcast_to(x[:, None, :], (experts, ROWS, tok))
        return x.reshape(experts * ROWS, tok)

    slot = spread(slot)
    high = spread(high.astype(F32))
    low = spread(low.astype(F32))
    row = lax.broadcasted_iota(jnp.int32, (experts * ROWS, tok), 0) & (ROWS - 1)
    for part in range(4):
        if part == 0:
            wanted = jnp.where(row < SLOTS, row, -1)
        else:
            wanted = jnp.where(row < SLOTS, -1, row - SLOTS + 2 * (part - 1))
        hit = slot == wanted.astype(F32)
        send_ref[:, part * tok : (part + 1) * tok] = jnp.where(hit, 1.0, 0.0).astype(BF)
        base = part * 2 * tok
        mix_ref[base : base + tok, :] = jnp.where(hit, high, 0.0).T.astype(BF)
        mix_ref[base + tok : base + 2 * tok, :] = jnp.where(hit, low, 0.0).T.astype(BF)


def route_tables(routes, weights, experts):
    topk, tok = routes.shape
    return pl.pallas_call(
        route_kernel,
        out_shape=(
            jax.ShapeDtypeStruct((experts * ROWS, 4 * tok), BF),
            jax.ShapeDtypeStruct((8 * tok, experts * ROWS), BF),
        ),
        in_specs=vmem_specs(2),
        out_specs=tuple(vmem_specs(2)),
        compiler_params=pltpu.CompilerParams(vmem_limit_bytes=16 * MIB),
        name="route_tables",
    )(routes, weights)


def middle_kernel(heads_ref, weight_ref, residual_ref, gain_ref, send_ref, mixed_ref, out_ref):
    tok, width = residual_ref.shape
    heads = heads_ref.shape[0] // tok
    joined = jnp.concatenate(
        [heads_ref[h * tok : (h + 1) * tok, :] for h in range(heads)], axis=1
    )
    tile = 256
    square = jnp.zeros((tok, tile), F32)
    for n in range(width // tile):
        cols = slice(n * tile, (n + 1) * tile)
        mixed = residual_ref[:, cols].astype(F32) + dot(joined, weight_ref[:, cols])
        mixed_ref[:, cols] = mixed
        square = square + mixed * mixed
    factor = lax.rsqrt(jnp.sum(square, axis=1, keepdims=True) / width + 1e-06)
    normed = (mixed_ref[...] * factor * gain_ref[...]).astype(BF)
    part = width // 4
    for q in range(3):
        rows = jnp.concatenate(
            [normed[:, q * part : (q + 1) * part], normed[:, 3 * part :]], axis=0
        )
        chosen = jnp.concatenate(
            [send_ref[:, 0:tok], send_ref[:, (q + 1) * tok : (q + 2) * tok]], axis=1
        )
        out_ref[:, q * part : (q + 1) * part] = dot(chosen, rows).astype(BF)


def middle(heads, weight, residual, gain, send):
    tok, width = residual.shape
    return pl.pallas_call(
        middle_kernel,
        out_shape=(
            jax.ShapeDtypeStruct((tok, width), F32),
            jax.ShapeDtypeStruct((send.shape[0], 3 * width // 4), BF),
        ),
        in_specs=vmem_specs(5),
        out_specs=tuple(vmem_specs(2)),
        compiler_params=pltpu.CompilerParams(vmem_limit_bytes=24 * MIB),
        name="middle",
    )(heads, weight, residual, gain, send)


def moved(x, shift):
    rows, cols = x.shape
    return pltpu.roll(x.reshape(rows // ROWS, ROWS, cols), shift, 1).reshape(rows, cols)


def experts_kernel(x_ref, gate_ref, up_ref, down_ref, out_ref, tail_ref, hidden_ref, last_ref):
    step = pl.program_id(0)
    rows = x_ref.shape[0]
    part = x_ref.shape[1] // 3
    tile = gate_ref.shape[1]
    gates = hidden_ref.shape[0]
    row = lax.broadcasted_iota(jnp.int32, (rows, part), 0) & (ROWS - 1)

    @pl.when(step == 0)
    def _():
        first = moved(x_ref[:, 0:part].astype(F32), 2)
        second = moved(x_ref[:, part : 2 * part].astype(F32), 4)
        third = moved(x_ref[:, 2 * part : 3 * part].astype(F32), 6)
        tail = jnp.where(row < 2, first, jnp.where(row < 4, second, third))
        tail_ref[...] = jnp.where(row < SLOTS, tail, 0.0).astype(BF)

    @pl.when(step < gates)
    def _():
        def times(w_ref):
            return dot(x_ref[...], w_ref[0 : 3 * part, :]) + dot(tail_ref[...], w_ref[3 * part :, :])

        gate = jnp.minimum(times(gate_ref), 7.0)
        up = jnp.clip(times(up_ref), -7.0, 7.0) + 1.0
        hidden_ref[step] = (up * gate * jax.nn.sigmoid(1.702 * gate)).astype(BF)

    def result():
        total = None
        for g in range(gates):
            term = dot(hidden_ref[g], down_ref[g * tile : (g + 1) * tile, :])
            total = term if total is None else total + term
        return total

    @pl.when(step == gates)
    def _():
        last_ref[...] = result()

    for q in range(3):

        @pl.when(step == gates + 1 + q)
        def _():
            out_ref[...] = jnp.where(
                row < SLOTS, result(), moved(last_ref[...], SLOTS - 2 * q)
            ).astype(BF)


def experts(x, gate_weight, up_weight, down_weight):
    rows = x.shape[0]
    width, hidden = gate_weight.shape
    part = width // 4
    tile = 256
    gates = hidden // tile

    def gate_map(i):
        return (0, jnp.minimum(i, gates - 1))

    def down_map(i):
        return (0, jnp.where(i <= gates, 3, i - gates - 1))

    def out_map(i):
        return (0, jnp.maximum(i - gates - 1, 0))

    return pl.pallas_call(
        experts_kernel,
        grid=(gates + 4,),
        out_shape=jax.ShapeDtypeStruct((rows, 3 * part), BF),
        in_specs=[
            pl.BlockSpec((rows, 3 * part), lambda i: (0, 0)),
            pl.BlockSpec((width, tile), gate_map),
            pl.BlockSpec((width, tile), gate_map),
            pl.BlockSpec((hidden, part), down_map),
        ],
        out_specs=pl.BlockSpec((rows, part), out_map),
        scratch_shapes=[
            pltpu.VMEM((rows, part), BF),
            pltpu.VMEM((gates, rows, tile), BF),
            pltpu.VMEM((rows, part), F32),
        ],
        compiler_params=pltpu.CompilerParams(vmem_limit_bytes=40 * MIB),
        name="experts",
    )(x, gate_weight, up_weight, down_weight)


def combine_kernel(mixed_ref, rows_ref, mix_ref, out_ref):
    tok, width = mixed_ref.shape
    part = width // 4
    last = mixed_ref[:, 3 * part :]
    for q in range(3):
        cols = slice(q * part, (q + 1) * part)
        weights = jnp.concatenate(
            [mix_ref[0 : 2 * tok, :], mix_ref[(q + 1) * 2 * tok : (q + 2) * 2 * tok, :]], axis=0
        )
        sums = dot(weights, rows_ref[:, cols])
        out_ref[:, cols] = (mixed_ref[:, cols] + sums[0:tok] + sums[tok : 2 * tok]).astype(BF)
        last = last + sums[2 * tok : 3 * tok] + sums[3 * tok :]
    out_ref[:, 3 * part :] = last.astype(BF)


def combine(mixed, rows, mix):
    return pl.pallas_call(
        combine_kernel,
        out_shape=jax.ShapeDtypeStruct(mixed.shape, BF),
        in_specs=vmem_specs(3),
        out_specs=pl.BlockSpec(memory_space=pltpu.VMEM),
        compiler_params=pltpu.CompilerParams(vmem_limit_bytes=24 * MIB),
        name="combine",
    )(mixed, rows, mix)


def exchange(x, axis, devices):
    pieces = x.reshape(devices, x.shape[0] // devices, x.shape[1])
    out = lax.all_to_all(pieces, axis, split_axis=0, concat_axis=0, tiled=True)
    return out.reshape(x.shape)


def on_device(
    query_first,
    key_first,
    query_second,
    key_second,
    value_rows,
    mix_lambda,
    head_gain,
    residual,
    out_weight,
    norm_gain,
    routes,
    route_weights,
    gate_weight,
    up_weight,
    down_weight,
):
    along = lax.axis_size("sp")
    everyone = along * lax.axis_size("dp")
    packed = pack_heads(
        query_first[0], key_first[0], query_second[0], key_second[0], value_rows[0]
    )
    qkv = exchange(packed, "sp", along)
    lam = lax.dynamic_slice_in_dim(mix_lambda, lax.axis_index("sp"), 1).reshape(1, 1)
    send, mix = route_tables(routes[0].T, route_weights[0].T, everyone)
    heads = exchange(attention(lam, head_gain.reshape(1, -1), qkv), "sp", along)
    mixed, outgoing = middle(heads, out_weight, residual[0], norm_gain.reshape(1, -1), send)
    received = exchange(outgoing, ("sp", "dp"), everyone)
    finished = experts(received, gate_weight[0], up_weight[0], down_weight[0])
    returned = exchange(finished, ("sp", "dp"), everyone)
    return combine(mixed, returned, mix)[None]


def solution(mesh):
    split = P("dp", "sp", None)
    held = P(("sp", "dp"), None, None)
    return jax.shard_map(
        on_device,
        mesh=mesh,
        in_specs=(split,) * 5 + (P(), P(), split, P(), P(), split, split) + (held,) * 3,
        out_specs=split,
        check_vma=False,
    )
```

```python
import functools

import jax
import jax.numpy as jnp
from jax import lax
from jax.experimental import pallas as pl
from jax.experimental.pallas import tpu as pltpu
from jax.sharding import PartitionSpec as P

BF = jnp.bfloat16
F32 = jnp.float32
LANES = 128
SLOTS = 6
ROWS = 8
MIB = 1024 * 1024


def dot(a, b, dims=((1,), (0,))):
    return lax.dot_general(a, b, (dims, ((), ())), preferred_element_type=F32)


def in_hbm(*arrays):
    return [pltpu.with_memory_space_constraint(a, pltpu.HBM) for a in arrays]


def vmem_specs(count):
    return [pl.BlockSpec(memory_space=pltpu.VMEM)] * count


def pack_kernel(q1_hbm, k1_hbm, q2_hbm, k2_hbm, v_hbm, out_ref, q1_ref, k1_ref, q2_ref, k2_ref, v_ref, sems):
    tok = q1_ref.shape[0]
    heads = v_ref.shape[1] // LANES
    half = LANES // 2
    pairs = ((q1_hbm, q1_ref), (q2_hbm, q2_ref), (k1_hbm, k1_ref), (k2_hbm, k2_ref), (v_hbm, v_ref))
    copies = [pltpu.make_async_copy(a, b, sems.at[i]) for i, (a, b) in enumerate(pairs)]
    for copy in copies:
        copy.start()
    for begin, (first, second) in ((0, (q1_ref, q2_ref)), (1, (k1_ref, k2_ref))):
        copies[2 * begin].wait()
        copies[2 * begin + 1].wait()
        lanes = slice(begin * LANES, (begin + 1) * LANES)
        for h in range(heads):
            cols = slice(h * half, (h + 1) * half)
            out_ref[h * tok : (h + 1) * tok, lanes] = jnp.concatenate(
                [first[:, cols], second[:, cols]], axis=1
            )
    copies[4].wait()
    for h in range(heads):
        out_ref[h * tok : (h + 1) * tok, 2 * LANES : 3 * LANES] = v_ref[
            :, h * LANES : (h + 1) * LANES
        ]


def pack_heads(q1, k1, q2, k2, v):
    tok = q1.shape[0]
    heads = v.shape[1] // LANES
    return pl.pallas_call(
        pack_kernel,
        out_shape=jax.ShapeDtypeStruct((heads * tok, 3 * LANES), BF),
        in_specs=[pl.BlockSpec(memory_space=pltpu.HBM)] * 5,
        out_specs=pl.BlockSpec(memory_space=pltpu.VMEM),
        scratch_shapes=[pltpu.VMEM(x.shape, BF) for x in (q1, k1, q2, k2, v)]
        + [pltpu.SemaphoreType.DMA((5,))],
        compiler_params=pltpu.CompilerParams(vmem_limit_bytes=8 * MIB),
        name="pack_heads",
    )(*in_hbm(q1, k1, q2, k2, v))


def attention_kernel(
    lam_ref, gain_ref, qkv_ref, *refs, block
):
    held = (len(refs) - 2) // 2
    out_ref, sems = refs[held], refs[-1]
    loads = [
        pltpu.make_async_copy(refs[i], refs[held + 1 + i], sems.at[i]) for i in range(held)
    ]
    for load in loads:
        load.start()
    length = qkv_ref.shape[0]
    half = LANES // 2
    scale = (half**-0.5) * 1.4426950408889634
    lane = lax.broadcasted_iota(jnp.int32, (block, LANES), 1)
    causal = lax.broadcasted_iota(jnp.int32, (2 * block, block), 1) <= (
        lax.broadcasted_iota(jnp.int32, (2 * block, block), 0) & (block - 1)
    )
    lam = lam_ref[lax.axis_index("sp")]
    gain = gain_ref[...]
    for step in range(length // block):
        rows = slice(step * block, (step + 1) * block)
        queries = qkv_ref[rows, 0:LANES]
        zero = jnp.zeros_like(queries)
        both = jnp.concatenate(
            [jnp.where(lane < half, queries, zero), jnp.where(lane < half, zero, queries)], axis=0
        )
        scores = []
        for c in range(step + 1):
            keys = qkv_ref[c * block : (c + 1) * block, LANES : 2 * LANES]
            s = dot(both, keys, ((1,), (1,)))
            if c == step:
                s = jnp.where(causal, s, -1e30)
            scores.append(s)
        top = functools.reduce(jnp.maximum, scores)
        top = jnp.max(top, axis=1, keepdims=True)
        total = None
        raw = None
        for c in range(step + 1):
            p = jnp.exp2((scores[c] - top) * scale)
            total = p if total is None else total + p
            values = qkv_ref[c * block : (c + 1) * block, 2 * LANES : 3 * LANES]
            part = dot(p.astype(BF), values)
            raw = part if raw is None else raw + part
        total = jnp.sum(total, axis=1, keepdims=True)
        normal = raw / total
        head = normal[:block] - lam * normal[block:]
        factor = lax.rsqrt(jnp.mean(head * head, axis=1, keepdims=True) + 1e-06)
        out_ref[rows, :] = (head * factor * gain).astype(BF)
    for load in loads:
        load.wait()


def attention(lam, gain, qkv, *weights):
    length = qkv.shape[0]
    return pl.pallas_call(
        functools.partial(attention_kernel, block=256),
        out_shape=(jax.ShapeDtypeStruct((length, LANES), BF),)
        + tuple(pltpu.VMEM(w.shape, BF) for w in weights),
        in_specs=[pl.BlockSpec(memory_space=pltpu.SMEM)]
        + vmem_specs(2)
        + [pl.BlockSpec(memory_space=pltpu.HBM)] * len(weights),
        out_specs=tuple(vmem_specs(1 + len(weights))),
        scratch_shapes=[pltpu.SemaphoreType.DMA((len(weights),))],
        compiler_params=pltpu.CompilerParams(vmem_limit_bytes=24 * MIB),
        name="attention",
    )(lam, gain, qkv, *in_hbm(*weights))


def spread(x):
    experts, tok = x.shape
    x = jnp.broadcast_to(x[:, None, :], (experts, ROWS, tok))
    return x.reshape(experts * ROWS, tok)


def slot_hits(slot):
    experts, tok = slot.shape
    slot = spread(slot)
    row = lax.broadcasted_iota(jnp.int32, (experts * ROWS, tok), 0) & (ROWS - 1)
    for part in range(4):
        if part == 0:
            wanted = jnp.where(row < SLOTS, row, -1)
        else:
            wanted = jnp.where(row < SLOTS, -1, row - SLOTS + 2 * (part - 1))
        yield slot == wanted.astype(F32)


def slot_table(routes_ref, experts):
    topk, tok = routes_ref.shape
    expert = lax.broadcasted_iota(jnp.int32, (experts, tok), 0)
    named = jnp.zeros((experts, tok), F32)
    hits = [expert == routes_ref[k : k + 1, :] for k in range(topk)]
    for hit in hits:
        named = jnp.where(hit, 1.0, named)
    before = lax.broadcasted_iota(jnp.int32, (tok, tok), 0) < lax.broadcasted_iota(
        jnp.int32, (tok, tok), 1
    )
    rank = dot(named.astype(BF), jnp.where(before, 1.0, 0.0).astype(BF))
    return jnp.where(named > 0.0, rank, -9.0), hits


def mix_table(routes_ref, weights_ref, mix_ref):
    tok = routes_ref.shape[1]
    slot, hits = slot_table(routes_ref, mix_ref.shape[1] // ROWS)
    weight = jnp.zeros(slot.shape, F32)
    for k, hit in enumerate(hits):
        weight = jnp.where(hit, weights_ref[k : k + 1, :], weight)
    high = weight.astype(BF).astype(F32)
    low = spread(weight - high)
    high = spread(high)
    for part, hit in enumerate(slot_hits(slot)):
        base = part * 2 * tok
        mix_ref[base : base + tok, :] = jnp.where(hit, high, 0.0).T.astype(BF)
        mix_ref[base + tok : base + 2 * tok, :] = jnp.where(hit, low, 0.0).T.astype(BF)


def middle_kernel(
    heads_ref, weight_ref, residual_ref, gain_ref, routes_ref, mixed_ref, out_ref
):
    tok, width = residual_ref.shape
    heads = heads_ref.shape[0] // tok
    tile = 256
    slot, _ = slot_table(routes_ref, out_ref.shape[0] // ROWS)
    hits = [jnp.where(hit, 1.0, 0.0).astype(BF) for hit in slot_hits(slot)]
    joined = jnp.concatenate(
        [heads_ref[h * tok : (h + 1) * tok, :] for h in range(heads)], axis=1
    )
    square = jnp.zeros((tok, tile), F32)
    for n in range(width // tile):
        cols = slice(n * tile, (n + 1) * tile)
        mixed = residual_ref[:, cols].astype(F32) + dot(joined, weight_ref[:, cols])
        mixed_ref[:, cols] = mixed
        square = square + mixed * mixed
    factor = lax.rsqrt(jnp.sum(square, axis=1, keepdims=True) / width + 1e-06)
    normed = (mixed_ref[...] * factor * gain_ref[...]).astype(BF)
    part = width // 4
    for q in range(3):
        rows = jnp.concatenate(
            [normed[:, q * part : (q + 1) * part], normed[:, 3 * part :]], axis=0
        )
        chosen = jnp.concatenate([hits[0], hits[q + 1]], axis=1)
        out_ref[:, q * part : (q + 1) * part] = dot(chosen, rows).astype(BF)


def middle(heads, weight, residual, gain, routes, experts):
    tok, width = residual.shape
    return pl.pallas_call(
        middle_kernel,
        out_shape=(
            jax.ShapeDtypeStruct((tok, width), F32),
            jax.ShapeDtypeStruct((experts * ROWS, 3 * width // 4), BF),
        ),
        in_specs=vmem_specs(5),
        out_specs=tuple(vmem_specs(2)),
        compiler_params=pltpu.CompilerParams(vmem_limit_bytes=24 * MIB),
        name="middle",
    )(heads, weight, residual, gain, routes)


def moved(x, shift):
    return x if shift == 0 else pltpu.roll(x, shift, 1)


def by_source(x):
    rows, cols = x.shape
    x = x.reshape(rows // (4 * ROWS), 4, ROWS, cols)
    return [x[:, i] for i in range(4)]


def together(pieces):
    groups, rows, cols = pieces[0].shape
    return jnp.stack(pieces, axis=1).reshape(groups * len(pieces) * rows, cols)


def compacted(parts):
    found = [by_source(part.astype(F32)) for part in parts]
    row = lax.broadcasted_iota(jnp.int32, found[0][0].shape, 1)
    main = []
    for a, b, c, d in found:
        b, c, d = moved(b, 6), moved(c, 4), moved(d, 2)
        main.append(
            together(
                [jnp.where(row < 6, a, b), jnp.where(row < 4, b, c), jnp.where(row < 2, c, d)]
            ).astype(BF)
        )
    tails = []
    for tile in range(3):
        total = None
        for place in range(4):
            piece = 4 * tile + place
            x = moved(found[piece % 3][piece // 3], (2 * place + 2) % ROWS)
            total = x if total is None else jnp.where(row < 2 * place, total, x)
        tails.append(total)
    return main + [together(tails).astype(BF)]


def expanded(part, tail, q):
    rows, cols = part.shape
    x = part.reshape(rows // 24, 3, ROWS, cols)
    t = tail.reshape(rows // 24, 3, ROWS, cols)
    first, second, third = x[:, 0], x[:, 1], x[:, 2]
    row = lax.broadcasted_iota(jnp.int32, first.shape, 1)
    slots = [
        first,
        moved(jnp.where(row < 4, second, first), 2),
        moved(jnp.where(row < 2, third, second), 4),
        moved(third, 6),
    ]
    out = []
    for source in range(4):
        piece = 3 * source + q
        ends = moved(t[:, piece // 4], (6 - 2 * (piece % 4)) % ROWS)
        out.append(jnp.where(row < SLOTS, slots[source], ends))
    return together(out).astype(BF)


def experts_kernel(
    x_ref, gate_ref, up_ref, down_ref, routes_ref, weights_ref, out_ref, mix_ref, rows_ref, hidden_ref
):
    width, hidden = gate_ref.shape
    part = width // 4
    tile = 256
    blocks = compacted([x_ref[:, q * part : (q + 1) * part] for q in range(3)])
    for q in range(4):
        rows_ref[:, q * part : (q + 1) * part] = blocks[q]
    for g in range(hidden // tile):
        cols = slice(g * tile, (g + 1) * tile)
        gate = jnp.minimum(dot(rows_ref[...], gate_ref[:, cols]), 7.0)
        up = jnp.clip(dot(rows_ref[...], up_ref[:, cols]), -7.0, 7.0) + 1.0
        hidden_ref[:, cols] = (up * gate * jax.nn.sigmoid(1.702 * gate)).astype(BF)
    tail = dot(hidden_ref[...], down_ref[:, 3 * part :])
    for q in range(3):
        cols = slice(q * part, (q + 1) * part)
        out_ref[:, cols] = expanded(dot(hidden_ref[...], down_ref[:, cols]), tail, q)
    mix_table(routes_ref, weights_ref, mix_ref)


def experts(x, gate_weight, up_weight, down_weight, routes, weights):
    rows = x.shape[0]
    width, hidden = gate_weight.shape
    held = rows * SLOTS // ROWS
    return pl.pallas_call(
        experts_kernel,
        out_shape=(
            jax.ShapeDtypeStruct(x.shape, BF),
            pltpu.VMEM((8 * routes.shape[1], rows), BF),
        ),
        in_specs=vmem_specs(6),
        out_specs=tuple(vmem_specs(2)),
        scratch_shapes=[
            pltpu.VMEM((held, width), BF),
            pltpu.VMEM((held, hidden), BF),
        ],
        compiler_params=pltpu.CompilerParams(vmem_limit_bytes=30 * MIB),
        name="experts",
    )(x, gate_weight, up_weight, down_weight, routes, weights)


def combine_kernel(mixed_ref, rows_ref, mix_ref, out_ref):
    tok, width = mixed_ref.shape
    part = width // 4
    last = mixed_ref[:, 3 * part :]
    for q in range(3):
        cols = slice(q * part, (q + 1) * part)
        weights = jnp.concatenate(
            [mix_ref[0 : 2 * tok, :], mix_ref[(q + 1) * 2 * tok : (q + 2) * 2 * tok, :]], axis=0
        )
        sums = dot(weights, rows_ref[:, cols])
        out_ref[:, cols] = (mixed_ref[:, cols] + sums[0:tok] + sums[tok : 2 * tok]).astype(BF)
        last = last + sums[2 * tok : 3 * tok] + sums[3 * tok :]
    out_ref[:, 3 * part :] = last.astype(BF)


def combine(mixed, rows, mix):
    return pl.pallas_call(
        combine_kernel,
        out_shape=jax.ShapeDtypeStruct(mixed.shape, BF),
        in_specs=vmem_specs(3),
        out_specs=pl.BlockSpec(memory_space=pltpu.VMEM),
        compiler_params=pltpu.CompilerParams(vmem_limit_bytes=24 * MIB),
        name="combine",
    )(mixed, rows, mix)


def exchange(x, axis, devices):
    pieces = x.reshape(devices, x.shape[0] // devices, x.shape[1])
    out = lax.all_to_all(pieces, axis, split_axis=0, concat_axis=0, tiled=True)
    return out.reshape(x.shape)


def on_device(
    query_first,
    key_first,
    query_second,
    key_second,
    value_rows,
    mix_lambda,
    head_gain,
    residual,
    out_weight,
    norm_gain,
    routes,
    route_weights,
    gate_weight,
    up_weight,
    down_weight,
):
    along = lax.axis_size("sp")
    everyone = along * lax.axis_size("dp")
    packed = pack_heads(
        query_first[0], key_first[0], query_second[0], key_second[0], value_rows[0]
    )
    qkv = exchange(packed, "sp", along)
    chosen, shares = routes[0].T, route_weights[0].T
    head, weight, gates, ups, downs = attention(
        mix_lambda,
        head_gain.reshape(1, -1),
        qkv,
        out_weight,
        gate_weight[0],
        up_weight[0],
        down_weight[0],
    )
    heads = exchange(head, "sp", along)
    gain = norm_gain.reshape(1, -1)
    mixed, outgoing = middle(heads, weight, residual[0], gain, chosen, everyone)
    received = exchange(outgoing, ("sp", "dp"), everyone)
    finished, mix = experts(received, gates, ups, downs, chosen, shares)
    returned = exchange(finished, ("sp", "dp"), everyone)
    return combine(mixed, returned, mix)[None]


def solution(mesh):
    split = P("dp", "sp", None)
    held = P(("sp", "dp"), None, None)
    return jax.shard_map(
        on_device,
        mesh=mesh,
        in_specs=(split,) * 5 + (P(), P(), split, P(), P(), split, split) + (held,) * 3,
        out_specs=split,
        check_vma=False,
    )
```

```python
import functools

import jax
import jax.numpy as jnp
from jax import lax
from jax.experimental import pallas as pl
from jax.experimental.pallas import tpu as pltpu
from jax.sharding import PartitionSpec as P

BF = jnp.bfloat16
F32 = jnp.float32
LANES = 128
SLOTS = 6
ROWS = 8
MIB = 1024 * 1024


def dot(a, b, dims=((1,), (0,))):
    return lax.dot_general(a, b, (dims, ((), ())), preferred_element_type=F32)


def in_hbm(*arrays):
    return [pltpu.with_memory_space_constraint(a, pltpu.HBM) for a in arrays]


def vmem_specs(count):
    return [pl.BlockSpec(memory_space=pltpu.VMEM)] * count


def pack_kernel(q1_hbm, k1_hbm, q2_hbm, k2_hbm, v_hbm, out_ref, q1_ref, k1_ref, q2_ref, k2_ref, v_ref, sems):
    tok = q1_ref.shape[0]
    heads = v_ref.shape[1] // LANES
    half = LANES // 2
    pairs = ((q1_hbm, q1_ref), (q2_hbm, q2_ref), (k1_hbm, k1_ref), (k2_hbm, k2_ref), (v_hbm, v_ref))
    copies = [pltpu.make_async_copy(a, b, sems.at[i]) for i, (a, b) in enumerate(pairs)]
    for copy in copies:
        copy.start()
    for begin, (first, second) in ((0, (q1_ref, q2_ref)), (1, (k1_ref, k2_ref))):
        copies[2 * begin].wait()
        copies[2 * begin + 1].wait()
        lanes = slice(begin * LANES, (begin + 1) * LANES)
        for h in range(heads):
            cols = slice(h * half, (h + 1) * half)
            out_ref[h * tok : (h + 1) * tok, lanes] = jnp.concatenate(
                [first[:, cols], second[:, cols]], axis=1
            )
    copies[4].wait()
    for h in range(heads):
        out_ref[h * tok : (h + 1) * tok, 2 * LANES : 3 * LANES] = v_ref[
            :, h * LANES : (h + 1) * LANES
        ]


def pack_heads(q1, k1, q2, k2, v):
    tok = q1.shape[0]
    heads = v.shape[1] // LANES
    return pl.pallas_call(
        pack_kernel,
        out_shape=jax.ShapeDtypeStruct((heads * tok, 3 * LANES), BF),
        in_specs=[pl.BlockSpec(memory_space=pltpu.HBM)] * 5,
        out_specs=pl.BlockSpec(memory_space=pltpu.VMEM),
        scratch_shapes=[pltpu.VMEM(x.shape, BF) for x in (q1, k1, q2, k2, v)]
        + [pltpu.SemaphoreType.DMA((5,))],
        compiler_params=pltpu.CompilerParams(vmem_limit_bytes=8 * MIB),
        name="pack_heads",
    )(*in_hbm(q1, k1, q2, k2, v))


def attention_kernel(
    lam_ref, gain_ref, qkv_ref, *refs, block
):
    held = (len(refs) - 2) // 2
    out_ref, sems = refs[held], refs[-1]
    loads = [
        pltpu.make_async_copy(refs[i], refs[held + 1 + i], sems.at[i]) for i in range(held)
    ]
    for load in loads:
        load.start()
    length = qkv_ref.shape[0]
    half = LANES // 2
    scale = (half**-0.5) * 1.4426950408889634
    lane = lax.broadcasted_iota(jnp.int32, (block, LANES), 1)
    causal = lax.broadcasted_iota(jnp.int32, (2 * block, block), 1) <= (
        lax.broadcasted_iota(jnp.int32, (2 * block, block), 0) & (block - 1)
    )
    lam = lam_ref[lax.axis_index("sp")]
    gain = gain_ref[...]
    steps = length // block
    ones = jnp.ones((block, LANES), BF)

    def both_maps(step):
        queries = qkv_ref[step * block : (step + 1) * block, 0:LANES]
        zero = jnp.zeros_like(queries)
        return jnp.concatenate(
            [jnp.where(lane < half, queries, zero), jnp.where(lane < half, zero, queries)], axis=0
        )

    def score(both, step, c):
        s = dot(both, qkv_ref[c * block : (c + 1) * block, LANES : 2 * LANES], ((1,), (1,)))
        return jnp.where(causal, s, -1e30) if c == step else s

    following = [score(both_maps(0), 0, 0)]
    for step in range(steps):
        rows = slice(step * block, (step + 1) * block)
        scores, following = following, []
        top = jnp.max(functools.reduce(jnp.maximum, scores), axis=1, keepdims=True)
        both = both_maps(step + 1) if step + 1 < steps else None
        raw = None
        probs = []
        for c in range(step + 2):
            if both is not None:
                following.append(score(both, step + 1, c))
            if c <= step:
                p = jnp.exp2((scores[c] - top) * scale).astype(BF)
                values = qkv_ref[c * block : (c + 1) * block, 2 * LANES : 3 * LANES]
                part = dot(p, jnp.concatenate([values, ones], axis=1))
                raw = part if raw is None else raw + part
        normal = raw[:, :LANES] / raw[:, LANES : LANES + 1]
        head = normal[:block] - lam * normal[block:]
        factor = lax.rsqrt(jnp.mean(head * head, axis=1, keepdims=True) + 1e-06)
        out_ref[rows, :] = (head * factor * gain).astype(BF)
    for load in loads:
        load.wait()


def attention(lam, gain, qkv, *weights):
    length = qkv.shape[0]
    return pl.pallas_call(
        functools.partial(attention_kernel, block=256),
        out_shape=(jax.ShapeDtypeStruct((length, LANES), BF),)
        + tuple(pltpu.VMEM(w.shape, BF) for w in weights),
        in_specs=[pl.BlockSpec(memory_space=pltpu.SMEM)]
        + vmem_specs(2)
        + [pl.BlockSpec(memory_space=pltpu.HBM)] * len(weights),
        out_specs=tuple(vmem_specs(1 + len(weights))),
        scratch_shapes=[pltpu.SemaphoreType.DMA((len(weights),))],
        compiler_params=pltpu.CompilerParams(vmem_limit_bytes=24 * MIB),
        name="attention",
    )(lam, gain, qkv, *in_hbm(*weights))


def spread(x):
    experts, tok = x.shape
    x = jnp.broadcast_to(x[:, None, :], (experts, ROWS, tok))
    return x.reshape(experts * ROWS, tok)


def slot_hits(slot):
    experts, tok = slot.shape
    slot = spread(slot)
    row = lax.broadcasted_iota(jnp.int32, (experts * ROWS, tok), 0) & (ROWS - 1)
    for part in range(4):
        if part == 0:
            wanted = jnp.where(row < SLOTS, row, -1)
        else:
            wanted = jnp.where(row < SLOTS, -1, row - SLOTS + 2 * (part - 1))
        yield slot == wanted.astype(F32)


def slot_table(routes_ref, experts):
    topk, tok = routes_ref.shape
    expert = lax.broadcasted_iota(jnp.int32, (experts, tok), 0)
    named = jnp.zeros((experts, tok), F32)
    hits = [expert == routes_ref[k : k + 1, :] for k in range(topk)]
    for hit in hits:
        named = jnp.where(hit, 1.0, named)
    before = lax.broadcasted_iota(jnp.int32, (tok, tok), 0) < lax.broadcasted_iota(
        jnp.int32, (tok, tok), 1
    )
    rank = dot(named.astype(BF), jnp.where(before, 1.0, 0.0).astype(BF))
    return jnp.where(named > 0.0, rank, -9.0), hits


def mix_table(routes_ref, weights_ref, mix_ref):
    tok = routes_ref.shape[1]
    slot, hits = slot_table(routes_ref, mix_ref.shape[1] // ROWS)
    weight = jnp.zeros(slot.shape, F32)
    for k, hit in enumerate(hits):
        weight = jnp.where(hit, weights_ref[k : k + 1, :], weight)
    weight = spread(weight)
    for part, hit in enumerate(slot_hits(slot)):
        mix_ref[part * tok : (part + 1) * tok, :] = jnp.where(hit, weight, 0.0).T.astype(BF)


def middle_kernel(
    heads_ref, weight_ref, residual_ref, gain_ref, routes_ref, mixed_ref, out_ref
):
    tok, width = residual_ref.shape
    heads = heads_ref.shape[0] // tok
    tile = 256
    slot, _ = slot_table(routes_ref, out_ref.shape[0] // ROWS)
    hits = [jnp.where(hit, 1.0, 0.0).astype(BF) for hit in slot_hits(slot)]
    joined = jnp.concatenate(
        [heads_ref[h * tok : (h + 1) * tok, :] for h in range(heads)], axis=1
    )
    square = jnp.zeros((tok, tile), F32)
    for n in range(width // tile):
        cols = slice(n * tile, (n + 1) * tile)
        mixed = residual_ref[:, cols].astype(F32) + dot(joined, weight_ref[:, cols])
        mixed_ref[:, cols] = mixed
        square = square + mixed * mixed
    factor = lax.rsqrt(jnp.sum(square, axis=1, keepdims=True) / width + 1e-06)
    normed = (mixed_ref[...] * factor * gain_ref[...]).astype(BF)
    part = width // 4
    for q in range(3):
        rows = jnp.concatenate(
            [normed[:, q * part : (q + 1) * part], normed[:, 3 * part :]], axis=0
        )
        chosen = jnp.concatenate([hits[0], hits[q + 1]], axis=1)
        out_ref[:, q * part : (q + 1) * part] = dot(chosen, rows).astype(BF)


def middle(heads, weight, residual, gain, routes, experts):
    tok, width = residual.shape
    return pl.pallas_call(
        middle_kernel,
        out_shape=(
            jax.ShapeDtypeStruct((tok, width), F32),
            jax.ShapeDtypeStruct((experts * ROWS, 3 * width // 4), BF),
        ),
        in_specs=vmem_specs(5),
        out_specs=tuple(vmem_specs(2)),
        compiler_params=pltpu.CompilerParams(vmem_limit_bytes=24 * MIB),
        name="middle",
    )(heads, weight, residual, gain, routes)


def moved(x, shift):
    return x if shift == 0 else pltpu.roll(x, shift, 1)


def by_source(x):
    rows, cols = x.shape
    x = x.reshape(rows // (4 * ROWS), 4, ROWS, cols)
    return [x[:, i] for i in range(4)]


def together(pieces):
    groups, rows, cols = pieces[0].shape
    return jnp.stack(pieces, axis=1).reshape(groups * len(pieces) * rows, cols)


def compacted(parts):
    found = [by_source(part.astype(F32)) for part in parts]
    row = lax.broadcasted_iota(jnp.int32, found[0][0].shape, 1)
    main = []
    for a, b, c, d in found:
        b, c, d = moved(b, 6), moved(c, 4), moved(d, 2)
        main.append(
            together(
                [jnp.where(row < 6, a, b), jnp.where(row < 4, b, c), jnp.where(row < 2, c, d)]
            ).astype(BF)
        )
    tails = []
    for tile in range(3):
        total = None
        for place in range(4):
            piece = 4 * tile + place
            x = moved(found[piece % 3][piece // 3], (2 * place + 2) % ROWS)
            total = x if total is None else jnp.where(row < 2 * place, total, x)
        tails.append(total)
    return main + [together(tails).astype(BF)]


def expanded(part, tail, q):
    rows, cols = part.shape
    x = part.reshape(rows // 24, 3, ROWS, cols)
    t = tail.reshape(rows // 24, 3, ROWS, cols)
    first, second, third = x[:, 0], x[:, 1], x[:, 2]
    row = lax.broadcasted_iota(jnp.int32, first.shape, 1)
    slots = [
        first,
        moved(jnp.where(row < 4, second, first), 2),
        moved(jnp.where(row < 2, third, second), 4),
        moved(third, 6),
    ]
    out = []
    for source in range(4):
        piece = 3 * source + q
        ends = moved(t[:, piece // 4], (6 - 2 * (piece % 4)) % ROWS)
        out.append(jnp.where(row < SLOTS, slots[source], ends))
    return together(out).astype(BF)


def experts_kernel(
    x_ref, gate_ref, up_ref, down_ref, routes_ref, weights_ref, out_ref, mix_ref, rows_ref, hidden_ref
):
    width, hidden = gate_ref.shape
    part = width // 4
    tile = 256
    blocks = compacted([x_ref[:, q * part : (q + 1) * part] for q in range(3)])
    for q in range(4):
        rows_ref[:, q * part : (q + 1) * part] = blocks[q]
    for g in range(hidden // tile):
        cols = slice(g * tile, (g + 1) * tile)
        gate = jnp.minimum(dot(rows_ref[...], gate_ref[:, cols]), 7.0)
        up = jnp.clip(dot(rows_ref[...], up_ref[:, cols]), -7.0, 7.0) + 1.0
        hidden_ref[:, cols] = (up * gate * jax.nn.sigmoid(1.702 * gate)).astype(BF)
    tail = dot(hidden_ref[...], down_ref[:, 3 * part :])
    for q in range(3):
        cols = slice(q * part, (q + 1) * part)
        out_ref[:, cols] = expanded(dot(hidden_ref[...], down_ref[:, cols]), tail, q)
    mix_table(routes_ref, weights_ref, mix_ref)


def experts(x, gate_weight, up_weight, down_weight, routes, weights):
    rows = x.shape[0]
    width, hidden = gate_weight.shape
    held = rows * SLOTS // ROWS
    return pl.pallas_call(
        experts_kernel,
        out_shape=(
            jax.ShapeDtypeStruct(x.shape, BF),
            pltpu.VMEM((4 * routes.shape[1], rows), BF),
        ),
        in_specs=vmem_specs(6),
        out_specs=tuple(vmem_specs(2)),
        scratch_shapes=[
            pltpu.VMEM((held, width), BF),
            pltpu.VMEM((held, hidden), BF),
        ],
        compiler_params=pltpu.CompilerParams(vmem_limit_bytes=30 * MIB),
        name="experts",
    )(x, gate_weight, up_weight, down_weight, routes, weights)


def combine_kernel(mixed_ref, rows_ref, mix_ref, out_ref):
    tok, width = mixed_ref.shape
    part = width // 4
    last = mixed_ref[:, 3 * part :]
    for q in range(3):
        cols = slice(q * part, (q + 1) * part)
        weights = jnp.concatenate(
            [mix_ref[0:tok, :], mix_ref[(q + 1) * tok : (q + 2) * tok, :]], axis=0
        )
        sums = dot(weights, rows_ref[:, cols])
        out_ref[:, cols] = (mixed_ref[:, cols] + sums[:tok]).astype(BF)
        last = last + sums[tok:]
    out_ref[:, 3 * part :] = last.astype(BF)


def combine(mixed, rows, mix):
    return pl.pallas_call(
        combine_kernel,
        out_shape=jax.ShapeDtypeStruct(mixed.shape, BF),
        in_specs=vmem_specs(3),
        out_specs=pl.BlockSpec(memory_space=pltpu.VMEM),
        compiler_params=pltpu.CompilerParams(vmem_limit_bytes=24 * MIB),
        name="combine",
    )(mixed, rows, mix)


def exchange(x, axis, devices):
    pieces = x.reshape(devices, x.shape[0] // devices, x.shape[1])
    out = lax.all_to_all(pieces, axis, split_axis=0, concat_axis=0, tiled=True)
    return out.reshape(x.shape)


def on_device(
    query_first,
    key_first,
    query_second,
    key_second,
    value_rows,
    mix_lambda,
    head_gain,
    residual,
    out_weight,
    norm_gain,
    routes,
    route_weights,
    gate_weight,
    up_weight,
    down_weight,
):
    along = lax.axis_size("sp")
    everyone = along * lax.axis_size("dp")
    packed = pack_heads(
        query_first[0], key_first[0], query_second[0], key_second[0], value_rows[0]
    )
    qkv = exchange(packed, "sp", along)
    chosen, shares = routes[0].T, route_weights[0].T
    head, weight, gates, ups, downs = attention(
        mix_lambda,
        head_gain.reshape(1, -1),
        qkv,
        out_weight,
        gate_weight[0],
        up_weight[0],
        down_weight[0],
    )
    heads = exchange(head, "sp", along)
    gain = norm_gain.reshape(1, -1)
    mixed, outgoing = middle(heads, weight, residual[0], gain, chosen, everyone)
    received = exchange(outgoing, ("sp", "dp"), everyone)
    finished, mix = experts(received, gates, ups, downs, chosen, shares)
    returned = exchange(finished, ("sp", "dp"), everyone)
    return combine(mixed, returned, mix)[None]


def solution(mesh):
    split = P("dp", "sp", None)
    held = P(("sp", "dp"), None, None)
    return jax.shard_map(
        on_device,
        mesh=mesh,
        in_specs=(split,) * 5 + (P(), P(), split, P(), P(), split, split) + (held,) * 3,
        out_specs=split,
        check_vma=False,
    )
```

```python
import functools

import jax
import jax.numpy as jnp
from jax import lax
from jax.experimental import pallas as pl
from jax.experimental.pallas import tpu as pltpu
from jax.sharding import PartitionSpec as P

BF = jnp.bfloat16
F32 = jnp.float32
LANES = 128
SLOTS = 6
ROWS = 8
MIB = 1024 * 1024


def dot(a, b, dims=((1,), (0,))):
    return lax.dot_general(a, b, (dims, ((), ())), preferred_element_type=F32)


def in_hbm(*arrays):
    return [pltpu.with_memory_space_constraint(a, pltpu.HBM) for a in arrays]


def vmem_specs(count):
    return [pl.BlockSpec(memory_space=pltpu.VMEM)] * count


def pack_kernel(q1_hbm, k1_hbm, q2_hbm, k2_hbm, v_hbm, out_ref, q1_ref, k1_ref, q2_ref, k2_ref, v_ref, sems):
    tok = q1_ref.shape[0]
    heads = v_ref.shape[1] // LANES
    half = LANES // 2
    pairs = ((q1_hbm, q1_ref), (q2_hbm, q2_ref), (k1_hbm, k1_ref), (k2_hbm, k2_ref), (v_hbm, v_ref))
    copies = [pltpu.make_async_copy(a, b, sems.at[i]) for i, (a, b) in enumerate(pairs)]
    for copy in copies:
        copy.start()
    for begin, (first, second) in ((0, (q1_ref, q2_ref)), (1, (k1_ref, k2_ref))):
        copies[2 * begin].wait()
        copies[2 * begin + 1].wait()
        lanes = slice(begin * LANES, (begin + 1) * LANES)
        for h in range(heads):
            cols = slice(h * half, (h + 1) * half)
            out_ref[h * tok : (h + 1) * tok, lanes] = jnp.concatenate(
                [first[:, cols], second[:, cols]], axis=1
            )
    copies[4].wait()
    for h in range(heads):
        out_ref[h * tok : (h + 1) * tok, 2 * LANES : 3 * LANES] = v_ref[
            :, h * LANES : (h + 1) * LANES
        ]


def pack_heads(q1, k1, q2, k2, v):
    tok = q1.shape[0]
    heads = v.shape[1] // LANES
    return pl.pallas_call(
        pack_kernel,
        out_shape=jax.ShapeDtypeStruct((heads * tok, 3 * LANES), BF),
        in_specs=[pl.BlockSpec(memory_space=pltpu.HBM)] * 5,
        out_specs=pl.BlockSpec(memory_space=pltpu.VMEM),
        scratch_shapes=[pltpu.VMEM(x.shape, BF) for x in (q1, k1, q2, k2, v)]
        + [pltpu.SemaphoreType.DMA((5,))],
        compiler_params=pltpu.CompilerParams(vmem_limit_bytes=8 * MIB),
        name="pack_heads",
    )(*in_hbm(q1, k1, q2, k2, v))


def attention_kernel(
    lam_ref, gain_ref, qkv_ref, *refs, block
):
    held = (len(refs) - 2) // 2
    out_ref, sems = refs[held], refs[-1]
    loads = [
        pltpu.make_async_copy(refs[i], refs[held + 1 + i], sems.at[i]) for i in range(held)
    ]
    for load in loads:
        load.start()
    length = qkv_ref.shape[0]
    half = LANES // 2
    scale = (half**-0.5) * 1.4426950408889634
    lane = lax.broadcasted_iota(jnp.int32, (block, LANES), 1)
    causal = lax.broadcasted_iota(jnp.int32, (2 * block, block), 1) <= (
        lax.broadcasted_iota(jnp.int32, (2 * block, block), 0) & (block - 1)
    )
    lam = lam_ref[lax.axis_index("sp")]
    gain = gain_ref[...]
    steps = length // block
    ones = jnp.ones((block, LANES), BF)

    def both_maps(step):
        queries = qkv_ref[step * block : (step + 1) * block, 0:LANES]
        zero = jnp.zeros_like(queries)
        return jnp.concatenate(
            [jnp.where(lane < half, queries, zero), jnp.where(lane < half, zero, queries)], axis=0
        )

    def score(both, step, c):
        s = dot(both, qkv_ref[c * block : (c + 1) * block, LANES : 2 * LANES], ((1,), (1,)))
        return jnp.where(causal, s, -1e30) if c == step else s

    following = [score(both_maps(0), 0, 0)]
    for step in range(steps):
        rows = slice(step * block, (step + 1) * block)
        scores, following = following, []
        top = jnp.max(functools.reduce(jnp.maximum, scores), axis=1, keepdims=True)
        both = both_maps(step + 1) if step + 1 < steps else None
        raw = None
        probs = []
        for c in range(step + 2):
            if both is not None:
                following.append(score(both, step + 1, c))
            if c <= step:
                p = jnp.exp2((scores[c] - top) * scale).astype(BF)
                values = qkv_ref[c * block : (c + 1) * block, 2 * LANES : 3 * LANES]
                part = dot(p, jnp.concatenate([values, ones], axis=1))
                raw = part if raw is None else raw + part
        normal = raw[:, :LANES] / raw[:, LANES : LANES + 1]
        head = normal[:block] - lam * normal[block:]
        factor = lax.rsqrt(jnp.mean(head * head, axis=1, keepdims=True) + 1e-06)
        out_ref[rows, :] = (head * factor * gain).astype(BF)
    for load in loads:
        load.wait()


def attention(lam, gain, qkv, *weights):
    length = qkv.shape[0]
    return pl.pallas_call(
        functools.partial(attention_kernel, block=256),
        out_shape=(jax.ShapeDtypeStruct((length, LANES), BF),)
        + tuple(pltpu.VMEM(w.shape, BF) for w in weights),
        in_specs=[pl.BlockSpec(memory_space=pltpu.SMEM)]
        + vmem_specs(2)
        + [pl.BlockSpec(memory_space=pltpu.HBM)] * len(weights),
        out_specs=tuple(vmem_specs(1 + len(weights))),
        scratch_shapes=[pltpu.SemaphoreType.DMA((len(weights),))],
        compiler_params=pltpu.CompilerParams(vmem_limit_bytes=24 * MIB),
        name="attention",
    )(lam, gain, qkv, *in_hbm(*weights))


def spread(x):
    experts, tok = x.shape
    x = jnp.broadcast_to(x[:, None, :], (experts, ROWS, tok))
    return x.reshape(experts * ROWS, tok)


def slot_hits(slot):
    experts, tok = slot.shape
    slot = spread(slot)
    row = lax.broadcasted_iota(jnp.int32, (experts * ROWS, tok), 0) & (ROWS - 1)
    for part in range(4):
        if part == 0:
            wanted = jnp.where(row < SLOTS, row, -1)
        else:
            wanted = jnp.where(row < SLOTS, -1, row - SLOTS + 2 * (part - 1))
        yield slot == wanted.astype(F32)


def slot_table(routes_ref, experts):
    topk, tok = routes_ref.shape
    expert = lax.broadcasted_iota(jnp.int32, (experts, tok), 0)
    named = jnp.zeros((experts, tok), F32)
    hits = [expert == routes_ref[k : k + 1, :] for k in range(topk)]
    for hit in hits:
        named = jnp.where(hit, 1.0, named)
    before = lax.broadcasted_iota(jnp.int32, (tok, tok), 0) < lax.broadcasted_iota(
        jnp.int32, (tok, tok), 1
    )
    rank = dot(named.astype(BF), jnp.where(before, 1.0, 0.0).astype(BF))
    return jnp.where(named > 0.0, rank, -9.0), hits


def mix_table(routes_ref, weights_ref, mix_ref):
    tok = routes_ref.shape[1]
    slot, hits = slot_table(routes_ref, mix_ref.shape[1] // ROWS)
    weight = jnp.zeros(slot.shape, F32)
    for k, hit in enumerate(hits):
        weight = jnp.where(hit, weights_ref[k : k + 1, :], weight)
    weight = spread(weight)
    for part, hit in enumerate(slot_hits(slot)):
        mix_ref[part * tok : (part + 1) * tok, :] = jnp.where(hit, weight, 0.0).T.astype(BF)


def middle_kernel(
    heads_ref, weight_ref, residual_ref, gain_ref, routes_ref, mixed_ref, out_ref
):
    tok, width = residual_ref.shape
    heads = heads_ref.shape[0] // tok
    tile = 256
    slot, _ = slot_table(routes_ref, out_ref.shape[0] // ROWS)
    hits = [jnp.where(hit, 1.0, 0.0).astype(BF) for hit in slot_hits(slot)]
    joined = jnp.concatenate(
        [heads_ref[h * tok : (h + 1) * tok, :] for h in range(heads)], axis=1
    )
    square = jnp.zeros((tok, tile), F32)
    for n in range(width // tile):
        cols = slice(n * tile, (n + 1) * tile)
        mixed = residual_ref[:, cols].astype(F32) + dot(joined, weight_ref[:, cols])
        mixed_ref[:, cols] = mixed
        square = square + mixed * mixed
    factor = lax.rsqrt(jnp.sum(square, axis=1, keepdims=True) / width + 1e-06)
    normed = (mixed_ref[...] * factor * gain_ref[...]).astype(BF)
    part = width // 4
    for q in range(3):
        rows = jnp.concatenate(
            [normed[:, q * part : (q + 1) * part], normed[:, 3 * part :]], axis=0
        )
        chosen = jnp.concatenate([hits[0], hits[q + 1]], axis=1)
        out_ref[:, q * part : (q + 1) * part] = dot(chosen, rows).astype(BF)


def middle(heads, weight, residual, gain, routes, experts):
    tok, width = residual.shape
    return pl.pallas_call(
        middle_kernel,
        out_shape=(
            jax.ShapeDtypeStruct((tok, width), F32),
            jax.ShapeDtypeStruct((experts * ROWS, 3 * width // 4), BF),
        ),
        in_specs=vmem_specs(5),
        out_specs=tuple(vmem_specs(2)),
        compiler_params=pltpu.CompilerParams(vmem_limit_bytes=24 * MIB),
        name="middle",
    )(heads, weight, residual, gain, routes)


def moved(x, shift):
    return x if shift == 0 else pltpu.roll(x, shift, 1)


def by_source(x):
    rows, cols = x.shape
    x = x.reshape(rows // (4 * ROWS), 4, ROWS, cols)
    return [x[:, i] for i in range(4)]


def together(pieces):
    groups, rows, cols = pieces[0].shape
    return jnp.stack(pieces, axis=1).reshape(groups * len(pieces) * rows, cols)


def compacted(parts):
    found = [by_source(part.astype(F32)) for part in parts]
    row = lax.broadcasted_iota(jnp.int32, found[0][0].shape, 1)
    main = []
    for a, b, c, d in found:
        b, c, d = moved(b, 6), moved(c, 4), moved(d, 2)
        main.append(
            together(
                [jnp.where(row < 6, a, b), jnp.where(row < 4, b, c), jnp.where(row < 2, c, d)]
            ).astype(BF)
        )
    tails = []
    for tile in range(3):
        total = None
        for place in range(4):
            piece = 4 * tile + place
            x = moved(found[piece % 3][piece // 3], (2 * place + 2) % ROWS)
            total = x if total is None else jnp.where(row < 2 * place, total, x)
        tails.append(total)
    return main + [together(tails).astype(BF)]


def expanded(part, tail, q):
    rows, cols = part.shape
    x = part.reshape(rows // 24, 3, ROWS, cols)
    t = tail.reshape(rows // 24, 3, ROWS, cols)
    first, second, third = x[:, 0], x[:, 1], x[:, 2]
    row = lax.broadcasted_iota(jnp.int32, first.shape, 1)
    slots = [
        first,
        moved(jnp.where(row < 4, second, first), 2),
        moved(jnp.where(row < 2, third, second), 4),
        moved(third, 6),
    ]
    out = []
    for source in range(4):
        piece = 3 * source + q
        ends = moved(t[:, piece // 4], (6 - 2 * (piece % 4)) % ROWS)
        out.append(jnp.where(row < SLOTS, slots[source], ends))
    return together(out).astype(BF)


def experts_kernel(
    x_ref, gate_ref, up_ref, down_ref, routes_ref, weights_ref, out_ref, mix_ref, rows_ref, hidden_ref
):
    width, hidden = gate_ref.shape
    part = width // 4
    tile = 256
    blocks = compacted([x_ref[:, q * part : (q + 1) * part] for q in range(3)])
    for q in range(4):
        rows_ref[:, q * part : (q + 1) * part] = blocks[q]
    for g in range(hidden // tile):
        cols = slice(g * tile, (g + 1) * tile)
        gate = jnp.minimum(dot(rows_ref[...], gate_ref[:, cols]), 7.0)
        up = jnp.clip(dot(rows_ref[...], up_ref[:, cols]), -7.0, 7.0) + 1.0
        hidden_ref[:, cols] = (up * gate * jax.nn.sigmoid(1.702 * gate)).astype(BF)
    tail = dot(hidden_ref[...], down_ref[:, 3 * part :])
    for q in range(3):
        cols = slice(q * part, (q + 1) * part)
        out_ref[:, cols] = expanded(dot(hidden_ref[...], down_ref[:, cols]), tail, q)
    mix_table(routes_ref, weights_ref, mix_ref)


def experts(x, gate_weight, up_weight, down_weight, routes, weights):
    rows = x.shape[0]
    width, hidden = gate_weight.shape
    held = rows * SLOTS // ROWS
    return pl.pallas_call(
        experts_kernel,
        out_shape=(
            jax.ShapeDtypeStruct(x.shape, BF),
            pltpu.VMEM((4 * routes.shape[1], rows), BF),
        ),
        in_specs=vmem_specs(6),
        out_specs=tuple(vmem_specs(2)),
        scratch_shapes=[
            pltpu.VMEM((held, width), BF),
            pltpu.VMEM((held, hidden), BF),
        ],
        compiler_params=pltpu.CompilerParams(vmem_limit_bytes=30 * MIB),
        name="experts",
    )(x, gate_weight, up_weight, down_weight, routes, weights)


def combine_kernel(mixed_ref, rows_ref, mix_ref, out_hbm, out_ref, sems):
    tok, width = mixed_ref.shape
    part = width // 4
    copies = []
    for q in range(4):
        cols = slice(q * part, (q + 1) * part)
        copies.append(pltpu.make_async_copy(out_ref.at[:, cols], out_hbm.at[:, cols], sems.at[q]))
    last = mixed_ref[:, 3 * part :]
    for q in range(3):
        cols = slice(q * part, (q + 1) * part)
        weights = jnp.concatenate(
            [mix_ref[0:tok, :], mix_ref[(q + 1) * tok : (q + 2) * tok, :]], axis=0
        )
        sums = dot(weights, rows_ref[:, cols])
        out_ref[:, cols] = (mixed_ref[:, cols] + sums[:tok]).astype(BF)
        copies[q].start()
        last = last + sums[tok:]
    out_ref[:, 3 * part :] = last.astype(BF)
    copies[3].start()
    for copy in copies:
        copy.wait()


def combine(mixed, rows, mix):
    return pl.pallas_call(
        combine_kernel,
        out_shape=jax.ShapeDtypeStruct(mixed.shape, BF),
        in_specs=vmem_specs(3),
        out_specs=pl.BlockSpec(memory_space=pltpu.HBM),
        scratch_shapes=[pltpu.VMEM(mixed.shape, BF), pltpu.SemaphoreType.DMA((4,))],
        compiler_params=pltpu.CompilerParams(vmem_limit_bytes=24 * MIB),
        name="combine",
    )(mixed, rows, mix)


def exchange(x, axis, devices):
    pieces = x.reshape(devices, x.shape[0] // devices, x.shape[1])
    out = lax.all_to_all(pieces, axis, split_axis=0, concat_axis=0, tiled=True)
    return out.reshape(x.shape)


def on_device(
    query_first,
    key_first,
    query_second,
    key_second,
    value_rows,
    mix_lambda,
    head_gain,
    residual,
    out_weight,
    norm_gain,
    routes,
    route_weights,
    gate_weight,
    up_weight,
    down_weight,
):
    along = lax.axis_size("sp")
    everyone = along * lax.axis_size("dp")
    packed = pack_heads(
        query_first[0], key_first[0], query_second[0], key_second[0], value_rows[0]
    )
    qkv = exchange(packed, "sp", along)
    chosen, shares = routes[0].T, route_weights[0].T
    head, weight, gates, ups, downs = attention(
        mix_lambda,
        head_gain.reshape(1, -1),
        qkv,
        out_weight,
        gate_weight[0],
        up_weight[0],
        down_weight[0],
    )
    heads = exchange(head, "sp", along)
    gain = norm_gain.reshape(1, -1)
    mixed, outgoing = middle(heads, weight, residual[0], gain, chosen, everyone)
    received = exchange(outgoing, ("sp", "dp"), everyone)
    finished, mix = experts(received, gates, ups, downs, chosen, shares)
    returned = exchange(finished, ("sp", "dp"), everyone)
    return combine(mixed, returned, mix)[None]


def solution(mesh):
    split = P("dp", "sp", None)
    held = P(("sp", "dp"), None, None)
    return jax.shard_map(
        on_device,
        mesh=mesh,
        in_specs=(split,) * 5 + (P(), P(), split, P(), P(), split, split) + (held,) * 3,
        out_specs=split,
        check_vma=False,
    )
```

```python
import functools

import jax
import jax.numpy as jnp
from jax import lax
from jax.experimental import pallas as pl
from jax.experimental.pallas import tpu as pltpu
from jax.sharding import PartitionSpec as P

BF = jnp.bfloat16
F32 = jnp.float32
LANES = 128
SLOTS = 6
ROWS = 8
MIB = 1024 * 1024


def dot(a, b, dims=((1,), (0,))):
    return lax.dot_general(a, b, (dims, ((), ())), preferred_element_type=F32)


def in_hbm(*arrays):
    return [pltpu.with_memory_space_constraint(a, pltpu.HBM) for a in arrays]


def vmem_specs(count):
    return [pl.BlockSpec(memory_space=pltpu.VMEM)] * count


def pack_kernel(q1_hbm, k1_hbm, q2_hbm, k2_hbm, v_hbm, out_ref, q1_ref, k1_ref, q2_ref, k2_ref, v_ref, sems):
    tok = q1_ref.shape[0]
    heads = v_ref.shape[1] // LANES
    half = LANES // 2
    pairs = ((q1_hbm, q1_ref), (q2_hbm, q2_ref), (k1_hbm, k1_ref), (k2_hbm, k2_ref), (v_hbm, v_ref))
    copies = [pltpu.make_async_copy(a, b, sems.at[i]) for i, (a, b) in enumerate(pairs)]
    for copy in copies:
        copy.start()
    for begin, (first, second) in ((0, (q1_ref, q2_ref)), (1, (k1_ref, k2_ref))):
        copies[2 * begin].wait()
        copies[2 * begin + 1].wait()
        lanes = slice(begin * LANES, (begin + 1) * LANES)
        for h in range(heads):
            cols = slice(h * half, (h + 1) * half)
            out_ref[h * tok : (h + 1) * tok, lanes] = jnp.concatenate(
                [first[:, cols], second[:, cols]], axis=1
            )
    copies[4].wait()
    for h in range(heads):
        out_ref[h * tok : (h + 1) * tok, 2 * LANES : 3 * LANES] = v_ref[
            :, h * LANES : (h + 1) * LANES
        ]


def pack_heads(q1, k1, q2, k2, v):
    tok = q1.shape[0]
    heads = v.shape[1] // LANES
    return pl.pallas_call(
        pack_kernel,
        out_shape=jax.ShapeDtypeStruct((heads * tok, 3 * LANES), BF),
        in_specs=[pl.BlockSpec(memory_space=pltpu.HBM)] * 5,
        out_specs=pl.BlockSpec(memory_space=pltpu.VMEM),
        scratch_shapes=[pltpu.VMEM(x.shape, BF) for x in (q1, k1, q2, k2, v)]
        + [pltpu.SemaphoreType.DMA((5,))],
        compiler_params=pltpu.CompilerParams(vmem_limit_bytes=8 * MIB),
        name="pack_heads",
    )(*in_hbm(q1, k1, q2, k2, v))


def attention_kernel(
    lam_ref, gain_ref, qkv_ref, *refs, block
):
    held = (len(refs) - 3) // 2
    out_ref, flat_ref, sems = refs[held], refs[-2], refs[-1]
    loads = [
        pltpu.make_async_copy(refs[i], refs[held + 1 + i], sems.at[i]) for i in range(held)
    ]
    for load in loads:
        load.start()
    length = qkv_ref.shape[0]
    half = LANES // 2
    scale = (half**-0.5) * 1.4426950408889634
    lane = lax.broadcasted_iota(jnp.int32, (block, LANES), 1)
    causal = lax.broadcasted_iota(jnp.int32, (block, 2 * block), 0) <= (
        lax.broadcasted_iota(jnp.int32, (block, 2 * block), 1) & (block - 1)
    )
    lam = lam_ref[lax.axis_index("sp")]
    gain = gain_ref[...]
    steps = length // block
    for c in range(steps):
        keys = slice(c * block, (c + 1) * block)
        flat_ref[0:LANES, keys] = qkv_ref[keys, 2 * LANES : 3 * LANES].T
    flat_ref[LANES:, :] = jnp.ones((flat_ref.shape[0] - LANES, length), BF)

    def both_maps(step):
        queries = qkv_ref[step * block : (step + 1) * block, 0:LANES]
        zero = jnp.zeros_like(queries)
        return jnp.concatenate(
            [jnp.where(lane < half, queries, zero), jnp.where(lane < half, zero, queries)], axis=0
        )

    wide = 2 * block

    def pair_maps(pair):
        return jnp.concatenate([both_maps(2 * pair), both_maps(2 * pair + 1)], axis=0)

    def score(both, pair, c):
        keys = qkv_ref[c * block : (c + 1) * block, LANES : 2 * LANES]
        if c > 2 * pair:
            return jnp.where(causal, dot(keys, both[wide:], ((1,), (1,))), -1e30)
        s = dot(keys, both, ((1,), (1,)))
        if c == 2 * pair:
            s = jnp.concatenate([jnp.where(causal, s[:, :wide], -1e30), s[:, wide:]], axis=1)
        return s

    pairs = steps // 2
    both = pair_maps(0)
    following = [score(both, 0, 0), score(both, 0, 1)]
    for pair in range(pairs):
        scores, following = following, []
        top = jnp.max(functools.reduce(jnp.maximum, scores[:-1]), axis=0, keepdims=True)
        late = jnp.maximum(top[:, wide:], jnp.max(scores[-1], axis=0, keepdims=True))
        top = jnp.concatenate([top[:, :wide], late], axis=1)
        both = pair_maps(pair + 1) if pair + 1 < pairs else None
        raw = None
        for c in range(2 * pair + 4):
            if both is not None:
                following.append(score(both, pair + 1, c))
            if c < 2 * pair + 2:
                last = c == 2 * pair + 1
                p = jnp.exp2((scores[c] - (late if last else top)) * scale).astype(BF)
                part = dot(flat_ref[:, c * block : (c + 1) * block], p)
                if last:
                    raw = (raw[:, :wide], raw[:, wide:] + part)
                else:
                    raw = part if raw is None else raw + part
        for i in range(2):
            begin = (2 * pair + i) * block
            normal = raw[i][:LANES] / raw[i][LANES : LANES + 1]
            head = normal[:, :block] - lam * normal[:, block:]
            factor = lax.rsqrt(jnp.mean(head * head, axis=0, keepdims=True) + 1e-06)
            out_ref[begin : begin + block, :] = ((head * factor).T * gain).astype(BF)
    for load in loads:
        load.wait()


def attention(lam, gain, qkv, *weights):
    length = qkv.shape[0]
    return pl.pallas_call(
        functools.partial(attention_kernel, block=256),
        out_shape=(jax.ShapeDtypeStruct((length, LANES), BF),)
        + tuple(pltpu.VMEM(w.shape, BF) for w in weights),
        in_specs=[pl.BlockSpec(memory_space=pltpu.SMEM)]
        + vmem_specs(2)
        + [pl.BlockSpec(memory_space=pltpu.HBM)] * len(weights),
        out_specs=tuple(vmem_specs(1 + len(weights))),
        scratch_shapes=[
            pltpu.VMEM((LANES + 16, length), BF),
            pltpu.SemaphoreType.DMA((len(weights),)),
        ],
        compiler_params=pltpu.CompilerParams(vmem_limit_bytes=24 * MIB),
        name="attention",
    )(lam, gain, qkv, *in_hbm(*weights))


def spread(x):
    experts, tok = x.shape
    x = jnp.broadcast_to(x[:, None, :], (experts, ROWS, tok))
    return x.reshape(experts * ROWS, tok)


def slot_hits(slot):
    experts, tok = slot.shape
    slot = spread(slot)
    row = lax.broadcasted_iota(jnp.int32, (experts * ROWS, tok), 0) & (ROWS - 1)
    for part in range(4):
        if part == 0:
            wanted = jnp.where(row < SLOTS, row, -1)
        else:
            wanted = jnp.where(row < SLOTS, -1, row - SLOTS + 2 * (part - 1))
        yield slot == wanted.astype(F32)


def slot_table(routes_ref, experts):
    topk, tok = routes_ref.shape
    expert = lax.broadcasted_iota(jnp.int32, (experts, tok), 0)
    named = jnp.zeros((experts, tok), F32)
    hits = [expert == routes_ref[k : k + 1, :] for k in range(topk)]
    for hit in hits:
        named = jnp.where(hit, 1.0, named)
    before = lax.broadcasted_iota(jnp.int32, (tok, tok), 0) < lax.broadcasted_iota(
        jnp.int32, (tok, tok), 1
    )
    rank = dot(named.astype(BF), jnp.where(before, 1.0, 0.0).astype(BF))
    return jnp.where(named > 0.0, rank, -9.0), hits


def mix_table(routes_ref, weights_ref, mix_ref):
    tok = routes_ref.shape[1]
    slot, hits = slot_table(routes_ref, mix_ref.shape[1] // ROWS)
    weight = jnp.zeros(slot.shape, F32)
    for k, hit in enumerate(hits):
        weight = jnp.where(hit, weights_ref[k : k + 1, :], weight)
    weight = spread(weight)
    for part, hit in enumerate(slot_hits(slot)):
        mix_ref[part * tok : (part + 1) * tok, :] = jnp.where(hit, weight, 0.0).T.astype(BF)


def middle_kernel(
    heads_ref, weight_ref, residual_ref, gain_ref, routes_ref, mixed_ref, out_ref
):
    tok, width = residual_ref.shape
    heads = heads_ref.shape[0] // tok
    tile = 256
    slot, _ = slot_table(routes_ref, out_ref.shape[0] // ROWS)
    hits = [jnp.where(hit, 1.0, 0.0).astype(BF) for hit in slot_hits(slot)]
    joined = jnp.concatenate(
        [heads_ref[h * tok : (h + 1) * tok, :] for h in range(heads)], axis=1
    )
    square = jnp.zeros((tok, tile), F32)
    for n in range(width // tile):
        cols = slice(n * tile, (n + 1) * tile)
        mixed = residual_ref[:, cols].astype(F32) + dot(joined, weight_ref[:, cols])
        mixed_ref[:, cols] = mixed
        square = square + mixed * mixed
    factor = lax.rsqrt(jnp.sum(square, axis=1, keepdims=True) / width + 1e-06)
    normed = (mixed_ref[...] * factor * gain_ref[...]).astype(BF)
    part = width // 4
    for q in range(3):
        rows = jnp.concatenate(
            [normed[:, q * part : (q + 1) * part], normed[:, 3 * part :]], axis=0
        )
        chosen = jnp.concatenate([hits[0], hits[q + 1]], axis=1)
        out_ref[:, q * part : (q + 1) * part] = dot(chosen, rows).astype(BF)


def middle(heads, weight, residual, gain, routes, experts):
    tok, width = residual.shape
    return pl.pallas_call(
        middle_kernel,
        out_shape=(
            jax.ShapeDtypeStruct((tok, width), F32),
            jax.ShapeDtypeStruct((experts * ROWS, 3 * width // 4), BF),
        ),
        in_specs=vmem_specs(5),
        out_specs=tuple(vmem_specs(2)),
        compiler_params=pltpu.CompilerParams(vmem_limit_bytes=24 * MIB),
        name="middle",
    )(heads, weight, residual, gain, routes)


def moved(x, shift):
    return x if shift == 0 else pltpu.roll(x, shift, 1)


def by_source(x):
    rows, cols = x.shape
    x = x.reshape(rows // (4 * ROWS), 4, ROWS, cols)
    return [x[:, i] for i in range(4)]


def together(pieces):
    groups, rows, cols = pieces[0].shape
    return jnp.stack(pieces, axis=1).reshape(groups * len(pieces) * rows, cols)


def compacted(parts):
    found = [by_source(part.astype(F32)) for part in parts]
    row = lax.broadcasted_iota(jnp.int32, found[0][0].shape, 1)
    main = []
    for a, b, c, d in found:
        b, c, d = moved(b, 6), moved(c, 4), moved(d, 2)
        main.append(
            together(
                [jnp.where(row < 6, a, b), jnp.where(row < 4, b, c), jnp.where(row < 2, c, d)]
            ).astype(BF)
        )
    tails = []
    for tile in range(3):
        total = None
        for place in range(4):
            piece = 4 * tile + place
            x = moved(found[piece % 3][piece // 3], (2 * place + 2) % ROWS)
            total = x if total is None else jnp.where(row < 2 * place, total, x)
        tails.append(total)
    return main + [together(tails).astype(BF)]


def expanded(part, tail, q):
    rows, cols = part.shape
    x = part.reshape(rows // 24, 3, ROWS, cols)
    t = tail.reshape(rows // 24, 3, ROWS, cols)
    first, second, third = x[:, 0], x[:, 1], x[:, 2]
    row = lax.broadcasted_iota(jnp.int32, first.shape, 1)
    slots = [
        first,
        moved(jnp.where(row < 4, second, first), 2),
        moved(jnp.where(row < 2, third, second), 4),
        moved(third, 6),
    ]
    out = []
    for source in range(4):
        piece = 3 * source + q
        ends = moved(t[:, piece // 4], (6 - 2 * (piece % 4)) % ROWS)
        out.append(jnp.where(row < SLOTS, slots[source], ends))
    return together(out).astype(BF)


def experts_kernel(
    x_ref, gate_ref, up_ref, down_ref, routes_ref, weights_ref, out_ref, mix_ref, rows_ref, hidden_ref
):
    width, hidden = gate_ref.shape
    part = width // 4
    tile = 256
    blocks = compacted([x_ref[:, q * part : (q + 1) * part] for q in range(3)])
    for q in range(4):
        rows_ref[:, q * part : (q + 1) * part] = blocks[q]
    for g in range(hidden // tile):
        cols = slice(g * tile, (g + 1) * tile)
        gate = jnp.minimum(dot(rows_ref[...], gate_ref[:, cols]), 7.0)
        up = jnp.clip(dot(rows_ref[...], up_ref[:, cols]), -7.0, 7.0) + 1.0
        hidden_ref[:, cols] = (up * gate * jax.nn.sigmoid(1.702 * gate)).astype(BF)
    tail = dot(hidden_ref[...], down_ref[:, 3 * part :])
    for q in range(3):
        cols = slice(q * part, (q + 1) * part)
        out_ref[:, cols] = expanded(dot(hidden_ref[...], down_ref[:, cols]), tail, q)
    mix_table(routes_ref, weights_ref, mix_ref)


def experts(x, gate_weight, up_weight, down_weight, routes, weights):
    rows = x.shape[0]
    width, hidden = gate_weight.shape
    held = rows * SLOTS // ROWS
    return pl.pallas_call(
        experts_kernel,
        out_shape=(
            jax.ShapeDtypeStruct(x.shape, BF),
            pltpu.VMEM((4 * routes.shape[1], rows), BF),
        ),
        in_specs=vmem_specs(6),
        out_specs=tuple(vmem_specs(2)),
        scratch_shapes=[
            pltpu.VMEM((held, width), BF),
            pltpu.VMEM((held, hidden), BF),
        ],
        compiler_params=pltpu.CompilerParams(vmem_limit_bytes=30 * MIB),
        name="experts",
    )(x, gate_weight, up_weight, down_weight, routes, weights)


def combine_kernel(mixed_ref, rows_ref, mix_ref, out_ref):
    tok, width = mixed_ref.shape
    part = width // 4
    last = mixed_ref[:, 3 * part :]
    for q in range(3):
        cols = slice(q * part, (q + 1) * part)
        weights = jnp.concatenate(
            [mix_ref[0:tok, :], mix_ref[(q + 1) * tok : (q + 2) * tok, :]], axis=0
        )
        sums = dot(weights, rows_ref[:, cols])
        out_ref[:, cols] = (mixed_ref[:, cols] + sums[:tok]).astype(BF)
        last = last + sums[tok:]
    out_ref[:, 3 * part :] = last.astype(BF)


def combine(mixed, rows, mix):
    return pl.pallas_call(
        combine_kernel,
        out_shape=jax.ShapeDtypeStruct(mixed.shape, BF),
        in_specs=vmem_specs(3),
        out_specs=pl.BlockSpec(memory_space=pltpu.VMEM),
        compiler_params=pltpu.CompilerParams(vmem_limit_bytes=24 * MIB),
        name="combine",
    )(mixed, rows, mix)


def exchange(x, axis, devices):
    pieces = x.reshape(devices, x.shape[0] // devices, x.shape[1])
    out = lax.all_to_all(pieces, axis, split_axis=0, concat_axis=0, tiled=True)
    return out.reshape(x.shape)


def on_device(
    query_first,
    key_first,
    query_second,
    key_second,
    value_rows,
    mix_lambda,
    head_gain,
    residual,
    out_weight,
    norm_gain,
    routes,
    route_weights,
    gate_weight,
    up_weight,
    down_weight,
):
    along = lax.axis_size("sp")
    everyone = along * lax.axis_size("dp")
    packed = pack_heads(
        query_first[0], key_first[0], query_second[0], key_second[0], value_rows[0]
    )
    qkv = exchange(packed, "sp", along)
    chosen, shares = routes[0].T, route_weights[0].T
    head, weight, gates, ups, downs = attention(
        mix_lambda,
        head_gain.reshape(1, -1),
        qkv,
        out_weight,
        gate_weight[0],
        up_weight[0],
        down_weight[0],
    )
    heads = exchange(head, "sp", along)
    gain = norm_gain.reshape(1, -1)
    mixed, outgoing = middle(heads, weight, residual[0], gain, chosen, everyone)
    received = exchange(outgoing, ("sp", "dp"), everyone)
    finished, mix = experts(received, gates, ups, downs, chosen, shares)
    returned = exchange(finished, ("sp", "dp"), everyone)
    return combine(mixed, returned, mix)[None]


def solution(mesh):
    split = P("dp", "sp", None)
    held = P(("sp", "dp"), None, None)
    return jax.shard_map(
        on_device,
        mesh=mesh,
        in_specs=(split,) * 5 + (P(), P(), split, P(), P(), split, split) + (held,) * 3,
        out_specs=split,
        check_vma=False,
    )
```
